256 devices in a mesh: grp: 2 (over y), sp: 32 (over z, core), tp: 4 (over x).
Axes of the slice: x: 4, y: 2, z: 16, core: 2. Of those that a mesh axis runs over, the one named last changes fastest.
The devices are a block of a 4x16x16 slice.
Arguments:
- residual: bfloat16 [32768, 2048], P(('grp', 'sp', 'tp')), parts along dimension 0, may hold values from -6 to 6
- queries: bfloat16 [32768, 2048], P(('grp', 'sp'), 'tp'), parts along dimension 0, may hold values from -200 to 200
- key_heads: bfloat16 [32768, 256], P(('grp', 'sp'), 'tp'), parts along dimension 0, may hold values from -8 to 8
- value_heads: bfloat16 [32768, 256], P(('grp', 'sp'), 'tp'), parts along dimension 0, may hold values from -6 to 6
- documents: int32 [32768], P(('grp', 'sp')), parts along dimension 0, may hold values from 0 to 7, never falling along the last dimension, each value on 1 to 8192 neighbouring positions
- sink_logits: float32 [32], P('tp'), may hold values from 4 to 7
- out_weight: bfloat16 [2048, 2048], P('tp'), may hold values from -1 to 1
- norm_gain: bfloat16 [2048], replicated, may hold values from 0.099609375 to 1.8984375
- gate_weight: bfloat16 [2048, 5632], P('sp', 'tp'), may hold values from -0.125 to 0.125
- up_weight: bfloat16 [2048, 5632], P('sp', 'tp'), may hold values from -0.125 to 0.125
- down_weight: bfloat16 [2048, 5632], P('sp', 'tp'), may hold values from -0.078125 to 0.078125
Outputs:
- updated: bfloat16 [32768, 2048], P(('grp', 'sp', 'tp')), parts along dimension 0
The draws below stay inside these ranges and needn't reach their ends.
There are 2 independent parts, one for each index of `grp`. The reference program is written for one: setup_inputs(seed, part) draws one part's arguments, and reference() takes and returns one part's arrays. A program takes and returns all parts, laid end to end along the dimension named above; an argument that names none is the same for every part. Nothing has to cross between parts.
Inputs may be any that keep to these rules, and one draw needn't show every extreme that they name: `documents`: document numbers never fall along the sequence.
All inputs are finite; a program needn't handle non-finite values.
Results may differ from the reference program's by a relative error of at most 0.012.
Values may be sent and summed in bfloat16 or wider, within the bound.
No kernel may reach another device: no remote copies, remote signals or barrier semaphores. Data moves between devices by JAX's collectives and lax.ppermute only.
A program may use at most 128 MiB of HBM per device.

```python
import math
import jax
import jax.numpy as jnp
import numpy as np
from jax import lax

D = 2048
HD = 64
QH = 32
KVH = 4
FF = 5632
WINDOW = 128
TOK_DEV = 512
SEQ = 16384
DOCS = 8
N_TP = 4


def drawn_pair(key):
    key_first = jax.random.fold_in(key, 11)
    key_second = jax.random.fold_in(key, 12)
    keys_base = jax.random.normal(key_first, (SEQ, KVH * HD), jnp.float32)
    query_base = jax.random.normal(key_second, (SEQ, QH * HD), jnp.float32)
    keys_out = keys_base
    query_out = query_base
    return (query_out, keys_out)


def draw_queries(key, part):
    return drawn_pair(key)[0].astype(jnp.bfloat16)


def draw_key_heads(key, part):
    return drawn_pair(key)[1].astype(jnp.bfloat16)


def block_levels(key, extent, cuts, low, top_value):
    factor_of = 1.0
    for axis_at, blocks in cuts:
        steps = jax.random.uniform(jax.random.fold_in(jax.random.fold_in(key, 6), axis_at), (blocks,), jnp.float32, low / len(cuts), top_value / len(cuts))
        factor_of = factor_of * jnp.repeat(jnp.exp(steps), extent[axis_at] // blocks).reshape((-1,) + (1,) * (len(extent) - 1 - axis_at))
    return factor_of


def split_up(amount, total, reach, skew):
    portions = [(1 << 20) // math.isqrt(rank ** skew) + 1 for rank in range(2, amount + 1)]
    surplus, counts = total - reach - (amount - 1), [1] * (amount - 1)
    while surplus > 0:
        free = [i for i in range(amount - 1) if counts[i] < reach]
        mass, budget = sum([portions[i] for i in free]), surplus
        for i in free:
            addition = min(reach - counts[i], max(1, budget * portions[i] // mass), surplus)
            counts[i] = counts[i] + addition
            surplus = surplus - addition
    return np.array([reach] + counts)


def ragged_sizes(key, count, total, bound, lean):
    if count == 2:
        one = jax.random.randint(key, (), max(1, total - bound), min(bound, total - 1) + 1)
        return jnp.stack([one, total - one])
    lengths = jnp.asarray(split_up(count, total, bound, lean), jnp.int32)
    pairs = (count - 1) // 2
    donor, sink = lengths[1:1 + 2 * pairs:2], lengths[2:2 + 2 * pairs:2]
    room = jnp.minimum(donor - 1, bound - sink)
    moved = jax.random.randint(jax.random.fold_in(key, 1), (pairs,), 0, 1 << 20) % (room + 1)
    lengths = lengths.at[1:1 + 2 * pairs:2].set(donor - moved).at[2:2 + 2 * pairs:2].set(sink + moved)
    return lengths[jax.random.permutation(jax.random.fold_in(key, 2), count)]


def scatter_about(own_key, dims, scale, bound, pieces=(), kind=jnp.bfloat16):
    loudness = block_levels(own_key, dims, pieces, -0.22, 0.18) if pieces else 1.0
    entries = jax.random.normal(own_key, dims, jnp.float32) * scale * loudness
    return jnp.minimum(jnp.maximum(entries, -bound), bound).astype(kind)


def setup_inputs(seed: int = 0, part: int = 0) -> dict:
    streams_of = jax.random.split(jax.random.key(seed), 12)
    part_splits = jax.random.split(jax.random.fold_in(streams_of[11], part), 12)
    return {
        "residual": scatter_about(part_splits[0], (SEQ, D), 1.0, 6.0, ((0, 128),)),
        "queries": draw_queries(jax.random.fold_in(jax.random.fold_in(streams_of[11], part), 71), part),
        "key_heads": draw_key_heads(jax.random.fold_in(jax.random.fold_in(streams_of[11], part), 71), part),
        "value_heads": scatter_about(part_splits[3], (SEQ, KVH * HD), 1.0, 6.0, ((0, 32), (1, 4))),
        "documents": jnp.searchsorted(jnp.cumsum(ragged_sizes(part_splits[4], DOCS, SEQ, SEQ // 2, 2)), jnp.arange(SEQ), side="right").astype(jnp.int32),
        "sink_logits": jnp.clip(4.0 + 3.0 * jax.random.uniform(streams_of[5], (QH,), jnp.float32) ** block_levels(streams_of[5], (QH,), ((0, 4),), -0.2, 0.2), 4.0, 7.0),
        "out_weight": scatter_about(streams_of[6], (QH * HD, D), QH ** -0.5, 1.0, ((0, 4),)),
        "norm_gain": jnp.clip(1.0 + 0.18 * jax.random.normal(streams_of[7], (D,), jnp.float32), 0.099609375, 1.8984375).astype(jnp.bfloat16),
        "gate_weight": scatter_about(streams_of[8], (D, FF), D ** -0.5, 0.125, ((0, 32), (1, 4))),
        "up_weight": scatter_about(streams_of[9], (D, FF), D ** -0.5, 0.125, ((0, 32), (1, 4))),
        "down_weight": scatter_about(streams_of[10], (D, FF), FF ** -0.5, 0.078125, ((0, 32), (1, 4))),
    }


epsilon = 1e-06
masked = -1e+30

def reference(residual, queries, key_heads, value_heads, documents, sink_logits, out_weight, norm_gain, gate_weight, up_weight, down_weight):
    length = queries.shape[0]
    groups = QH // KVH
    blocks = length // TOK_DEV
    padded_keys = jnp.pad(key_heads, ((WINDOW, WINDOW), (0, 0)))
    padded_values = jnp.pad(value_heads, ((WINDOW, WINDOW), (0, 0)))
    padded_docs = jnp.pad(documents, (WINDOW, WINDOW))
    sink_table = sink_logits.astype(jnp.float32).reshape(KVH, groups)[:, :, None]

    def attend_block(block_index):
        row_start = (block_index * TOK_DEV).astype(jnp.int32)
        query_block = lax.dynamic_slice_in_dim(queries, row_start, TOK_DEV, 0).astype(jnp.float32).reshape(TOK_DEV, KVH, groups, HD)
        key_block = lax.dynamic_slice_in_dim(padded_keys, row_start, TOK_DEV + 2 * WINDOW, 0).astype(jnp.float32).reshape(-1, KVH, HD)
        value_block = lax.dynamic_slice_in_dim(padded_values, row_start, TOK_DEV + 2 * WINDOW, 0).astype(jnp.float32).reshape(-1, KVH, HD)
        query_docs = lax.dynamic_slice_in_dim(documents, row_start, TOK_DEV, 0)
        key_docs = lax.dynamic_slice_in_dim(padded_docs, row_start, TOK_DEV + 2 * WINDOW, 0)
        query_pos = row_start + jnp.arange(TOK_DEV, dtype=jnp.int32)
        key_pos = row_start - WINDOW + jnp.arange(TOK_DEV + 2 * WINDOW, dtype=jnp.int32)
        allowed = (jnp.abs(query_pos[:, None] - key_pos[None, :]) <= WINDOW) & (key_pos >= 0)[None, :] & (key_pos < length)[None, :] & (query_docs[:, None] == key_docs[None, :])
        scores = jnp.einsum('qkgd,jkd->kgqj', query_block, key_block) * HD ** (-0.5)
        scores = jnp.where(allowed[None, None], scores, masked)
        row_max = jnp.maximum(lax.optimization_barrier(jnp.max(scores, axis=-1)), sink_table)
        expo = jnp.exp(scores - row_max[..., None])
        total = lax.optimization_barrier(jnp.sum(expo, axis=-1)) + jnp.exp(sink_table - row_max)
        probs = (expo / total[..., None]).astype(jnp.bfloat16)
        mixed = jnp.einsum('kgqj,jkd->qkgd', probs.astype(jnp.float32), value_block)
        return mixed.reshape(TOK_DEV, QH * HD).astype(jnp.bfloat16)
    attended = lax.map(attend_block, jnp.arange(blocks, dtype=jnp.int32)).reshape(length, QH * HD)
    projected = jnp.dot(attended, out_weight, preferred_element_type=jnp.float32).astype(jnp.bfloat16)
    middle = (residual.astype(jnp.float32) + lax.optimization_barrier(projected).astype(jnp.float32)).astype(jnp.bfloat16)
    middle_wide = middle.astype(jnp.float32)
    scaled = middle_wide * lax.rsqrt(lax.optimization_barrier(jnp.mean(middle_wide * middle_wide, axis=-1, keepdims=True)) + epsilon)
    normed = (scaled * norm_gain.astype(jnp.float32)).astype(jnp.bfloat16)
    block_width = FF // N_TP

    def mix_block(block_index):
        row_start = (block_index * TOK_DEV).astype(jnp.int32)
        row_block = lax.dynamic_slice_in_dim(normed, row_start, TOK_DEV, 0)
        gate_value = jnp.dot(row_block, gate_weight, preferred_element_type=jnp.float32)
        up_value = jnp.dot(row_block, up_weight, preferred_element_type=jnp.float32)
        hidden = (jax.nn.silu(gate_value) * up_value).astype(jnp.bfloat16)
        summed = jnp.zeros((TOK_DEV, D), jnp.float32)
        for shard_index in range(N_TP):
            columns = hidden[:, shard_index * block_width:(shard_index + 1) * block_width]
            down_block = down_weight[:, shard_index * block_width:(shard_index + 1) * block_width]
            term = lax.dot_general(columns, down_block, (((1,), (1,)), ((), ())), preferred_element_type=jnp.float32).astype(jnp.bfloat16)
            summed = summed + lax.optimization_barrier(term).astype(jnp.float32)
        return summed.astype(jnp.bfloat16)
    mixer_out = lax.map(mix_block, jnp.arange(blocks, dtype=jnp.int32)).reshape(length, D)
    updated = middle.astype(jnp.float32) + 0.5 * lax.optimization_barrier(mixer_out).astype(jnp.float32)
    return updated.astype(jnp.bfloat16)
```

```python
import functools

import jax
import jax.numpy as jnp
from jax import lax
from jax.experimental import pallas as pl
from jax.experimental.pallas import tpu as pltpu
from jax.sharding import PartitionSpec as P

HD = 64
WINDOW = 128
LANES = 128

epsilon = 1e-06
masked = -1e30

VMEM = pl.BlockSpec(memory_space=pltpu.VMEM)
HBM = pl.BlockSpec(memory_space=pl.ANY)
LIMIT = pltpu.CompilerParams(vmem_limit_bytes=56 * 1024 * 1024)


def split_up(shard, length):
    return shard.reshape(length, shard.shape[0] // length, *shard.shape[1:])


def pack_body(gate, up, down, out):
    ff = gate.shape[1]
    for i in range(ff // LANES):
        at = slice(i * LANES, (i + 1) * LANES)
        out[:, 2 * i * LANES : (2 * i + 1) * LANES] = gate[:, at]
        out[:, (2 * i + 1) * LANES : (2 * i + 2) * LANES] = up[:, at]
    out[:, 2 * ff :] = down[...]


def pack(gate, up, down):
    rows, ff = gate.shape
    return pl.pallas_call(
        pack_body,
        out_shape=jax.ShapeDtypeStruct((rows, 3 * ff), gate.dtype),
        in_specs=[VMEM] * 3,
        out_specs=VMEM,
        name="pack",
    )(gate, up, down)


def down_part(hidden, weight):
    return lax.dot_general(
        hidden, weight, (((1,), (1,)), ((), ())), preferred_element_type=jnp.float32
    ).astype(jnp.bfloat16)


def first_body(width, x, w, hidden, part, wide, narrow, sems, sem):
    ff = hidden.shape[1]
    steps = [(a, min(a + 512, 2 * ff)) for a in range(0, 2 * ff, 512)]
    copies = [
        pltpu.make_async_copy(w.at[:, a:b], wide.at[:, a:b], sems.at[k])
        for k, (a, b) in enumerate(steps)
    ]
    last = pltpu.make_async_copy(w.at[0:width, 2 * ff :], narrow, sem)
    for c in copies:
        c.start()
    last.start()
    for c, (a, b) in zip(copies, steps):
        c.wait()
        both = jnp.dot(x[...], wide[:, a:b], preferred_element_type=jnp.float32)
        for k in range((b - a) // (2 * LANES)):
            gate = both[:, 2 * k * LANES : (2 * k + 1) * LANES]
            up = both[:, (2 * k + 1) * LANES : (2 * k + 2) * LANES]
            at = a // 2 + k * LANES
            hidden[:, at : at + LANES] = (gate / (1.0 + jnp.exp(-gate)) * up).astype(hidden.dtype)
    last.wait()
    part[...] = down_part(hidden[...], narrow[...])


def ffn_first(x, w, width):
    rows, d = x.shape
    ff = w.shape[1] // 3
    n = -(-2 * ff // 512)
    return pl.pallas_call(
        functools.partial(first_body, width),
        out_shape=(
            jax.ShapeDtypeStruct((rows, ff), x.dtype),
            jax.ShapeDtypeStruct((rows, width), x.dtype),
        ),
        in_specs=[VMEM, HBM],
        out_specs=(VMEM, VMEM),
        scratch_shapes=[
            pltpu.VMEM((d, 2 * ff), x.dtype),
            pltpu.VMEM((width, ff), x.dtype),
            pltpu.SemaphoreType.DMA((n,)),
            pltpu.SemaphoreType.DMA,
        ],
        compiler_params=LIMIT,
        cost_estimate=pl.CostEstimate(
            flops=2 * rows * ff * (2 * d + width), bytes_accessed=4 * d * ff + 4 * rows * d, transcendentals=rows * ff
        ),
        name="ffn_first",
    )(x, w)


def next_body(start, width, hidden, w, part, narrow, sem):
    ff = hidden.shape[1]
    copy = pltpu.make_async_copy(w.at[start : start + width, 2 * ff :], narrow, sem)
    copy.start()
    copy.wait()
    part[...] = down_part(hidden[...], narrow[...])


def ffn_next(hidden, w, start, width):
    rows, ff = hidden.shape
    return pl.pallas_call(
        functools.partial(next_body, start, width),
        out_shape=jax.ShapeDtypeStruct((rows, width), hidden.dtype),
        in_specs=[VMEM, HBM],
        out_specs=VMEM,
        scratch_shapes=[pltpu.VMEM((width, ff), hidden.dtype), pltpu.SemaphoreType.DMA],
        compiler_params=LIMIT,
        cost_estimate=pl.CostEstimate(
            flops=2 * rows * ff * width, bytes_accessed=2 * (rows + width) * ff, transcendentals=0
        ),
        name="ffn_next",
    )(hidden, w)


def finish_body(*refs):
    middle, parts, out = refs[0], refs[1:-1], refs[-1]
    at = 0
    for part in parts:
        width = part.shape[2]
        total = part[0].astype(jnp.float32)
        for k in range(1, part.shape[0]):
            total = total + part[k].astype(jnp.float32)
        mixed = total.astype(jnp.bfloat16).astype(jnp.float32)
        here = slice(at, at + width)
        out[:, here] = (middle[:, here].astype(jnp.float32) + 0.5 * mixed).astype(out.dtype)
        at += width


def finish(middle, parts):
    return pl.pallas_call(
        finish_body,
        out_shape=jax.ShapeDtypeStruct(middle.shape, middle.dtype),
        in_specs=[VMEM] * (1 + len(parts)),
        out_specs=VMEM,
        name="finish",
    )(middle, *parts)


def middle_body(residual, parts, gain, middle, normed):
    total = parts[0].astype(jnp.float32)
    for k in range(1, parts.shape[0]):
        total = total + parts[k].astype(jnp.float32)
    projected = total.astype(jnp.bfloat16).astype(jnp.float32)
    mid = (residual[...].astype(jnp.float32) + projected).astype(jnp.bfloat16)
    middle[...] = mid
    wide = mid.astype(jnp.float32)
    scaled = wide * lax.rsqrt(jnp.mean(wide * wide, axis=-1, keepdims=True) + epsilon)
    out = (scaled * gain[...].astype(jnp.float32)).astype(normed.dtype)
    for k in range(normed.shape[0]):
        normed[k] = out


def middle_and_normed(residual, parts, gain):
    rows, d = residual.shape
    return pl.pallas_call(
        middle_body,
        out_shape=(
            jax.ShapeDtypeStruct((rows, d), residual.dtype),
            jax.ShapeDtypeStruct((parts.shape[0], rows, d), residual.dtype),
        ),
        in_specs=[VMEM] * 3,
        out_specs=(VMEM, VMEM),
        name="middle",
    )(residual, parts, gain.reshape(1, d))


def exchanged(blocks):
    return lax.all_to_all(blocks, "tp", 0, 0, tiled=True)


def attention(queries, key_heads, value_heads, documents, sink_logits):
    tok_rows = queries.shape[0]
    q_local = queries.shape[1] // HD
    kv_local = key_heads.shape[1] // HD
    groups = q_local // kv_local
    size = lax.axis_size("sp")
    own_docs = documents.astype(jnp.bfloat16)
    keys_values = jnp.concatenate([key_heads, value_heads], axis=1)
    width = keys_values.shape[1]

    def edge(lo):
        docs = jnp.broadcast_to(own_docs[lo : lo + WINDOW].reshape(-1, width), (16, width))
        return jnp.concatenate([keys_values[lo : lo + WINDOW], docs], axis=0)

    up = [(i, i + 1) for i in range(size - 1)]
    down = [(j, i) for i, j in up]
    before = lax.ppermute(edge(tok_rows - WINDOW), "sp", up)
    after = lax.ppermute(edge(0), "sp", down)
    spread = jnp.concatenate([before[:WINDOW], keys_values, after[:WINDOW]], axis=0)
    spread_docs = jnp.concatenate([before[WINDOW], own_docs, after[WINDOW]])
    spread_keys, spread_values = spread[:, : kv_local * HD], spread[:, kv_local * HD :]
    offset = lax.axis_index("sp") * tok_rows
    total_length = tok_rows * size
    query_pos = offset + jnp.arange(tok_rows, dtype=jnp.int32)
    key_pos = offset - WINDOW + jnp.arange(tok_rows + 2 * WINDOW, dtype=jnp.int32)
    allowed = (
        (jnp.abs(query_pos[:, None] - key_pos[None, :]) <= WINDOW)
        & (key_pos >= 0)[None, :]
        & (key_pos < total_length)[None, :]
        & (own_docs[:, None] == spread_docs[None, :])
    )
    query_block = queries.reshape(tok_rows, kv_local, groups, HD)
    key_block = spread_keys.reshape(-1, kv_local, HD)
    value_block = spread_values.reshape(-1, kv_local, HD)
    scores = jnp.einsum(
        "qkgd,jkd->kgqj", query_block, key_block, preferred_element_type=jnp.float32
    ) * HD ** (-0.5)
    scores = jnp.where(allowed[None, None], scores, masked)
    sink_table = sink_logits.reshape(kv_local, groups)[:, :, None]
    row_max = jnp.maximum(jnp.max(scores, axis=-1), sink_table)
    expo = jnp.exp(scores - row_max[..., None])
    total = jnp.sum(expo, axis=-1) + jnp.exp(sink_table - row_max)
    probs = (expo / total[..., None]).astype(jnp.bfloat16)
    mixed = jnp.einsum("kgqj,jkd->qkgd", probs, value_block, preferred_element_type=jnp.float32)
    return mixed.reshape(tok_rows, q_local * HD).astype(jnp.bfloat16)


def on_device(
    residual,
    queries,
    key_heads,
    value_heads,
    documents,
    sink_logits,
    out_weight,
    norm_gain,
    gate_weight,
    up_weight,
    down_weight,
):
    n_tp = lax.axis_size("tp")
    d = residual.shape[1]
    whole = lax.all_gather(pack(gate_weight, up_weight, down_weight), "sp", axis=0, tiled=True)
    attended = attention(queries, key_heads, value_heads, documents, sink_logits)
    partial = jnp.dot(attended, out_weight, preferred_element_type=jnp.float32)
    parts = exchanged(split_up(partial.astype(jnp.bfloat16), n_tp))
    middle, copies = middle_and_normed(residual, parts, norm_gain)
    rows = exchanged(copies).reshape(-1, d)
    width = d // 4
    hidden, part = ffn_first(rows, whole, width)
    mixes = [exchanged(split_up(part, n_tp))]
    for k in range(1, 4):
        part = ffn_next(hidden, whole, k * width, width)
        mixes.append(exchanged(split_up(part, n_tp)))
    return finish(middle, mixes)


def solution(mesh):
    return jax.shard_map(
        on_device,
        mesh=mesh,
        in_specs=(
            P(("grp", "sp", "tp"), None),
            P(("grp", "sp"), "tp"),
            P(("grp", "sp"), "tp"),
            P(("grp", "sp"), "tp"),
            P(("grp", "sp")),
            P("tp"),
            P("tp", None),
            P(),
            P("sp", "tp"),
            P("sp", "tp"),
            P("sp", "tp"),
        ),
        out_specs=P(("grp", "sp", "tp"), None),
        check_vma=False,
    )
```

```python
import functools

import jax
import jax.numpy as jnp
from jax import lax
from jax.experimental import pallas as pl
from jax.experimental.pallas import tpu as pltpu
from jax.sharding import PartitionSpec as P

HD = 64
WINDOW = 128
LANES = 128
WIDE = 1536
TALL = 256

epsilon = 1e-06
masked = -1e30

VMEM = pl.BlockSpec(memory_space=pltpu.VMEM)
SMEM = pl.BlockSpec(memory_space=pltpu.SMEM)
HBM = pl.BlockSpec(memory_space=pl.ANY)
LIMIT = pltpu.CompilerParams(vmem_limit_bytes=56 * 1024 * 1024)


def split_up(shard, length):
    return shard.reshape(length, shard.shape[0] // length, *shard.shape[1:])


def pack_body(gate, up, out):
    for i in range(gate.shape[1] // LANES):
        at = slice(i * LANES, (i + 1) * LANES)
        out[:, 2 * i * LANES : (2 * i + 1) * LANES] = gate[:, at]
        out[:, (2 * i + 1) * LANES : (2 * i + 2) * LANES] = up[:, at]


def pack(gate, up):
    rows, ff = gate.shape
    return pl.pallas_call(
        pack_body,
        out_shape=jax.ShapeDtypeStruct((rows, 2 * ff), gate.dtype),
        in_specs=[VMEM] * 2,
        out_specs=VMEM,
        name="pack",
    )(gate, up)


def pair_body(side, own, other, out):
    out[side[0]] = own[...]
    out[1 - side[0]] = other[...]


def pair(side, own, other):
    return pl.pallas_call(
        pair_body,
        out_shape=jax.ShapeDtypeStruct((2, *own.shape), own.dtype),
        in_specs=[SMEM, VMEM, VMEM],
        out_specs=VMEM,
        name="pair",
    )(side, own, other)


def ring_of_pairs(shard):
    size = lax.axis_size("sp")
    pairs = size // 2
    side = lax.axis_index("sp") % 2
    around = [(i, (i + (2 if i % 2 == 0 else -2)) % size) for i in range(size)]
    swap = [(i, i ^ 1) for i in range(size)]
    block = pair(side.reshape(1), shard, lax.ppermute(shard, "sp", swap))
    kept, swapped = [block], []
    for step in range(1, pairs // 2 + 1):
        if 2 * step == pairs:
            block = lax.dynamic_index_in_dim(block, side, 0, keepdims=False)
        block = lax.ppermute(block, "sp", around)
        kept.append(block)
        swapped.append(lax.ppermute(block, "sp", swap))
    return kept, swapped


def ffn_body(n_kept, n_swapped, place, rows, w, *refs):
    blocks = refs[: n_kept + n_swapped]
    out, x, wide, narrow, hidden, xsem, wsems, dsems = refs[n_kept + n_swapped :]
    d, two_ff = wide.shape
    ff = two_ff // 2
    tokens = x.shape[0]
    pairs = d // narrow.shape[1] // 2
    here, side = place[0], place[1]
    way = 1 - 2 * side
    copies = []
    for k, block in enumerate(blocks):
        step = k if k < n_kept else k - n_kept + 1
        sign = -way if k < n_kept else way
        at = lax.rem(here + sign * step + pairs, pairs)
        if len(block.shape) == 3:
            target = narrow.at[pl.ds(2 * at, 2)]
        else:
            target = narrow.at[2 * at + (side if k < n_kept else 1 - side)]
        copies.append(pltpu.make_async_copy(block, target, dsems.at[k]))
    steps = [(a, min(a + WIDE, two_ff)) for a in range(0, two_ff, WIDE)]
    loads = [
        pltpu.make_async_copy(w.at[:, a:b], wide.at[:, a:b], wsems.at[k])
        for k, (a, b) in enumerate(steps)
    ]
    load_x = pltpu.make_async_copy(rows, x, xsem)
    load_x.start()
    for c in loads + copies:
        c.start()
    load_x.wait()
    for c, (a, b) in zip(loads, steps):
        c.wait()

        @pl.loop(0, tokens // TALL)
        def _(m, a=a, b=b):
            here = pl.ds(m * TALL, TALL)
            both = jnp.dot(x[here], wide[:, a:b], preferred_element_type=jnp.float32)
            for k in range((b - a) // (2 * LANES)):
                gate = both[:, 2 * k * LANES : (2 * k + 1) * LANES]
                up = both[:, (2 * k + 1) * LANES : (2 * k + 2) * LANES]
                at = a // 2 + k * LANES
                hidden[here, at : at + LANES] = (gate / (1.0 + jnp.exp(-gate)) * up).astype(
                    hidden.dtype
                )

    for c in copies:
        c.wait()
    half = narrow.shape[0] // 2
    for n in range(2):

        @pl.loop(0, tokens // TALL)
        def _(m, n=n):
            here = pl.ds(m * TALL, TALL)
            weight = narrow[n * half : (n + 1) * half].reshape(d // 2, ff)
            out[here, n * d // 2 : (n + 1) * d // 2] = lax.dot_general(
                hidden[here], weight, (((1,), (1,)), ((), ())), preferred_element_type=jnp.float32
            ).astype(out.dtype)


def ffn(rows, w, kept, swapped):
    tokens, d = rows.shape
    ff = w.shape[1] // 2
    shard = kept[0].shape[1]
    blocks = [*kept, *swapped]
    index = lax.axis_index("sp")
    place = jnp.stack([index // 2, index % 2]).astype(jnp.int32)
    n = -(-2 * ff // WIDE)
    return pl.pallas_call(
        functools.partial(ffn_body, len(kept), len(swapped)),
        out_shape=jax.ShapeDtypeStruct((tokens, d), rows.dtype),
        in_specs=[SMEM] + [HBM] * (2 + len(blocks)),
        out_specs=VMEM,
        scratch_shapes=[
            pltpu.VMEM((tokens, d), rows.dtype),
            pltpu.VMEM((d, 2 * ff), rows.dtype),
            pltpu.VMEM((d // shard, shard, ff), rows.dtype),
            pltpu.VMEM((tokens, ff), rows.dtype),
            pltpu.SemaphoreType.DMA,
            pltpu.SemaphoreType.DMA((n,)),
            pltpu.SemaphoreType.DMA((len(blocks),)),
        ],
        compiler_params=LIMIT,
        cost_estimate=pl.CostEstimate(
            flops=6 * tokens * ff * d, bytes_accessed=6 * d * ff + 4 * tokens * d, transcendentals=tokens * ff
        ),
        name="ffn",
    )(place, rows, w, *blocks)


def finish_body(*refs):
    middle, parts, out = refs[0], refs[1:-1], refs[-1]
    at = 0
    for part in parts:
        width = part.shape[2]
        total = part[0].astype(jnp.float32)
        for k in range(1, part.shape[0]):
            total = total + part[k].astype(jnp.float32)
        mixed = total.astype(jnp.bfloat16).astype(jnp.float32)
        here = slice(at, at + width)
        out[:, here] = (middle[:, here].astype(jnp.float32) + 0.5 * mixed).astype(out.dtype)
        at += width


def finish(middle, parts):
    return pl.pallas_call(
        finish_body,
        out_shape=jax.ShapeDtypeStruct(middle.shape, middle.dtype),
        in_specs=[VMEM] * (1 + len(parts)),
        out_specs=VMEM,
        name="finish",
    )(middle, *parts)


def middle_body(residual, parts, gain, middle, normed):
    total = parts[0].astype(jnp.float32)
    for k in range(1, parts.shape[0]):
        total = total + parts[k].astype(jnp.float32)
    projected = total.astype(jnp.bfloat16).astype(jnp.float32)
    mid = (residual[...].astype(jnp.float32) + projected).astype(jnp.bfloat16)
    middle[...] = mid
    wide = mid.astype(jnp.float32)
    scaled = wide * lax.rsqrt(jnp.mean(wide * wide, axis=-1, keepdims=True) + epsilon)
    out = (scaled * gain[...].astype(jnp.float32)).astype(normed.dtype)
    for k in range(normed.shape[0]):
        normed[k] = out


def middle_and_normed(residual, parts, gain):
    rows, d = residual.shape
    return pl.pallas_call(
        middle_body,
        out_shape=(
            jax.ShapeDtypeStruct((rows, d), residual.dtype),
            jax.ShapeDtypeStruct((parts.shape[0], rows, d), residual.dtype),
        ),
        in_specs=[VMEM] * 3,
        out_specs=(VMEM, VMEM),
        name="middle",
    )(residual, parts, gain.reshape(1, d))


def exchanged(blocks):
    return lax.all_to_all(blocks, "tp", 0, 0, tiled=True)


def attention(queries, key_heads, value_heads, documents, sink_logits):
    tok_rows = queries.shape[0]
    q_local = queries.shape[1] // HD
    kv_local = key_heads.shape[1] // HD
    groups = q_local // kv_local
    size = lax.axis_size("sp")
    own_docs = documents.astype(jnp.bfloat16)
    keys_values = jnp.concatenate([key_heads, value_heads], axis=1)
    width = keys_values.shape[1]

    def edge(lo):
        docs = jnp.broadcast_to(own_docs[lo : lo + WINDOW].reshape(-1, width), (16, width))
        return jnp.concatenate([keys_values[lo : lo + WINDOW], docs], axis=0)

    up = [(i, i + 1) for i in range(size - 1)]
    down = [(j, i) for i, j in up]
    before = lax.ppermute(edge(tok_rows - WINDOW), "sp", up)
    after = lax.ppermute(edge(0), "sp", down)
    spread = jnp.concatenate([before[:WINDOW], keys_values, after[:WINDOW]], axis=0)
    spread_docs = jnp.concatenate([before[WINDOW], own_docs, after[WINDOW]])
    spread_keys, spread_values = spread[:, : kv_local * HD], spread[:, kv_local * HD :]
    offset = lax.axis_index("sp") * tok_rows
    total_length = tok_rows * size
    query_pos = offset + jnp.arange(tok_rows, dtype=jnp.int32)
    key_pos = offset - WINDOW + jnp.arange(tok_rows + 2 * WINDOW, dtype=jnp.int32)
    allowed = (
        (jnp.abs(query_pos[:, None] - key_pos[None, :]) <= WINDOW)
        & (key_pos >= 0)[None, :]
        & (key_pos < total_length)[None, :]
        & (own_docs[:, None] == spread_docs[None, :])
    )
    query_block = queries.reshape(tok_rows, kv_local, groups, HD)
    key_block = spread_keys.reshape(-1, kv_local, HD)
    value_block = spread_values.reshape(-1, kv_local, HD)
    scores = jnp.einsum(
        "qkgd,jkd->kgqj", query_block, key_block, preferred_element_type=jnp.float32
    ) * HD ** (-0.5)
    scores = jnp.where(allowed[None, None], scores, masked)
    sink_table = sink_logits.reshape(kv_local, groups)[:, :, None]
    row_max = jnp.maximum(jnp.max(scores, axis=-1), sink_table)
    expo = jnp.exp(scores - row_max[..., None])
    total = jnp.sum(expo, axis=-1) + jnp.exp(sink_table - row_max)
    probs = (expo / total[..., None]).astype(jnp.bfloat16)
    mixed = jnp.einsum("kgqj,jkd->qkgd", probs, value_block, preferred_element_type=jnp.float32)
    return mixed.reshape(tok_rows, q_local * HD).astype(jnp.bfloat16)


def on_device(
    residual,
    queries,
    key_heads,
    value_heads,
    documents,
    sink_logits,
    out_weight,
    norm_gain,
    gate_weight,
    up_weight,
    down_weight,
):
    n_tp = lax.axis_size("tp")
    d = residual.shape[1]
    whole = lax.all_gather(pack(gate_weight, up_weight), "sp", axis=0, tiled=True)
    kept, swapped = ring_of_pairs(down_weight)
    attended = attention(queries, key_heads, value_heads, documents, sink_logits)
    partial = jnp.dot(attended, out_weight, preferred_element_type=jnp.float32)
    parts = exchanged(split_up(partial.astype(jnp.bfloat16), n_tp))
    middle, copies = middle_and_normed(residual, parts, norm_gain)
    rows = exchanged(copies).reshape(-1, d)
    mixed = exchanged(split_up(ffn(rows, whole, kept, swapped), n_tp))
    return finish(middle, [mixed])


def solution(mesh):
    return jax.shard_map(
        on_device,
        mesh=mesh,
        in_specs=(
            P(("grp", "sp", "tp"), None),
            P(("grp", "sp"), "tp"),
            P(("grp", "sp"), "tp"),
            P(("grp", "sp"), "tp"),
            P(("grp", "sp")),
            P("tp"),
            P("tp", None),
            P(),
            P("sp", "tp"),
            P("sp", "tp"),
            P("sp", "tp"),
        ),
        out_specs=P(("grp", "sp", "tp"), None),
        check_vma=False,
    )
```

```python
import functools

import jax
import jax.numpy as jnp
from jax import lax
from jax.experimental import pallas as pl
from jax.experimental.pallas import tpu as pltpu
from jax.sharding import PartitionSpec as P


HD = 64
WINDOW = 128
LANES = 128
WIDE = 1536
TALL = 256


epsilon = 1e-06
masked = -1e30

VMEM = pl.BlockSpec(memory_space=pltpu.VMEM)
SMEM = pl.BlockSpec(memory_space=pltpu.SMEM)
HBM = pl.BlockSpec(memory_space=pl.ANY)
LIMIT = pltpu.CompilerParams(vmem_limit_bytes=56 * 1024 * 1024)


def split_up(shard, length):
    return shard.reshape(length, shard.shape[0] // length, *shard.shape[1:])


def pack_body(gate, up, down, out):
    ff = gate.shape[1]
    for i in range(ff // LANES):
        at = slice(i * LANES, (i + 1) * LANES)
        out[:, 2 * i * LANES : (2 * i + 1) * LANES] = gate[:, at]
        out[:, (2 * i + 1) * LANES : (2 * i + 2) * LANES] = up[:, at]
    out[:, 2 * ff :] = down[...]


def pack(gate, up, down):
    rows, ff = gate.shape
    return pl.pallas_call(
        pack_body,
        out_shape=jax.ShapeDtypeStruct((rows, 3 * ff), gate.dtype),
        in_specs=[VMEM] * 3,
        out_specs=VMEM,
        name="pack",
    )(gate, up, down)


def pair_body(side, own, other, out):
    out[side[0]] = own[...]
    out[1 - side[0]] = other[...]


def pair(side, own, other):
    return pl.pallas_call(
        pair_body,
        out_shape=jax.ShapeDtypeStruct((2, *own.shape), own.dtype),
        in_specs=[SMEM, VMEM, VMEM],
        out_specs=VMEM,
        name="pair",
    )(side, own, other)


class Ring:
    def __init__(self, shard):
        size = lax.axis_size("sp")
        self.pairs = size // 2
        self.side = lax.axis_index("sp") % 2
        self.around = [(i, (i + (2 if i % 2 == 0 else -2)) % size) for i in range(size)]
        self.swap = [(i, i ^ 1) for i in range(size)]
        other = lax.ppermute(shard, "sp", self.swap)
        self.block = pair(self.side.reshape(1), shard, other)
        self.kept, self.swapped = [self.block], []

    def run(self):
        block = self.block
        for step in range(1, self.pairs // 2 + 1):
            if 2 * step == self.pairs:
                block = lax.dynamic_index_in_dim(block, self.side, 0, keepdims=False)
            block = lax.ppermute(block, "sp", self.around)
            self.kept.append(block)
            self.swapped.append(lax.ppermute(block, "sp", self.swap))


def ffn_body(n_kept, n_swapped, place, rows, *refs):
    blocks = refs[: n_kept + n_swapped]
    out, x, whole, hidden, xsem, sems = refs[n_kept + n_swapped :]
    d = x.shape[1]
    ff = hidden.shape[1]
    tokens = x.shape[0]
    pairs = whole.shape[0] // 2
    here, side = place[0], place[1]
    way = 1 - 2 * side
    copies = [pltpu.make_async_copy(rows, x, xsem)]
    for k, block in enumerate(blocks):
        step = k if k < n_kept else k - n_kept + 1
        sign = -way if k < n_kept else way
        at = lax.rem(here + sign * step + pairs, pairs)
        if len(block.shape) == 3:
            target = whole.at[pl.ds(2 * at, 2)]
        else:
            target = whole.at[2 * at + (side if k < n_kept else 1 - side)]
        copies.append(pltpu.make_async_copy(block, target, sems.at[k]))
    for c in copies:
        c.start()
    for c in copies:
        c.wait()
    for a in range(0, 2 * ff, WIDE):
        b = min(a + WIDE, 2 * ff)

        @pl.loop(0, tokens // TALL)
        def _(m, a=a, b=b):
            at = pl.ds(m * TALL, TALL)
            weight = whole[:, :, a:b].reshape(d, b - a)
            both = jnp.dot(x[at], weight, preferred_element_type=jnp.float32)
            for k in range((b - a) // (2 * LANES)):
                gate = both[:, 2 * k * LANES : (2 * k + 1) * LANES]
                up = both[:, (2 * k + 1) * LANES : (2 * k + 2) * LANES]
                lane = a // 2 + k * LANES
                hidden[at, lane : lane + LANES] = (gate / (1.0 + jnp.exp(-gate)) * up).astype(
                    hidden.dtype
                )

    half = whole.shape[0] // 2
    for n in range(2):

        @pl.loop(0, tokens // TALL)
        def _(m, n=n):
            at = pl.ds(m * TALL, TALL)
            weight = whole[n * half : (n + 1) * half, :, 2 * ff :].reshape(d // 2, ff)
            out[at, n * d // 2 : (n + 1) * d // 2] = lax.dot_general(
                hidden[at], weight, (((1,), (1,)), ((), ())), preferred_element_type=jnp.float32
            ).astype(out.dtype)


def ffn(rows, kept, swapped):
    tokens, d = rows.shape
    _, shard, three_ff = kept[0].shape
    ff = three_ff // 3
    blocks = [*kept, *swapped]
    index = lax.axis_index("sp")
    place = jnp.stack([index // 2, index % 2]).astype(jnp.int32)
    return pl.pallas_call(
        functools.partial(ffn_body, len(kept), len(swapped)),
        out_shape=jax.ShapeDtypeStruct((tokens, d), rows.dtype),
        in_specs=[SMEM] + [HBM] * (1 + len(blocks)),
        out_specs=VMEM,
        scratch_shapes=[
            pltpu.VMEM((tokens, d), rows.dtype),
            pltpu.VMEM((d // shard, shard, 3 * ff), rows.dtype),
            pltpu.VMEM((tokens, ff), rows.dtype),
            pltpu.SemaphoreType.DMA,
            pltpu.SemaphoreType.DMA((len(blocks),)),
        ],
        compiler_params=LIMIT,
        cost_estimate=pl.CostEstimate(
            flops=6 * tokens * ff * d, bytes_accessed=6 * d * ff + 4 * tokens * d, transcendentals=tokens * ff
        ),
        name="ffn",
    )(place, rows, *blocks)


def finish_body(*refs):
    middle, parts, out = refs[0], refs[1:-1], refs[-1]
    at = 0
    for part in parts:
        width = part.shape[2]
        total = part[0].astype(jnp.float32)
        for k in range(1, part.shape[0]):
            total = total + part[k].astype(jnp.float32)
        mixed = total.astype(jnp.bfloat16).astype(jnp.float32)
        here = slice(at, at + width)
        out[:, here] = (middle[:, here].astype(jnp.float32) + 0.5 * mixed).astype(out.dtype)
        at += width


def finish(middle, parts):
    return pl.pallas_call(
        finish_body,
        out_shape=jax.ShapeDtypeStruct(middle.shape, middle.dtype),
        in_specs=[VMEM] * (1 + len(parts)),
        out_specs=VMEM,
        name="finish",
    )(middle, *parts)


def middle_body(residual, parts, gain, middle, normed):
    total = parts[0].astype(jnp.float32)
    for k in range(1, parts.shape[0]):
        total = total + parts[k].astype(jnp.float32)
    projected = total.astype(jnp.bfloat16).astype(jnp.float32)
    mid = (residual[...].astype(jnp.float32) + projected).astype(jnp.bfloat16)
    middle[...] = mid
    wide = mid.astype(jnp.float32)
    scaled = wide * lax.rsqrt(jnp.mean(wide * wide, axis=-1, keepdims=True) + epsilon)
    out = (scaled * gain[...].astype(jnp.float32)).astype(normed.dtype)
    for k in range(normed.shape[0]):
        normed[k] = out


def middle_and_normed(residual, parts, gain):
    rows, d = residual.shape
    return pl.pallas_call(
        middle_body,
        out_shape=(
            jax.ShapeDtypeStruct((rows, d), residual.dtype),
            jax.ShapeDtypeStruct((parts.shape[0], rows, d), residual.dtype),
        ),
        in_specs=[VMEM] * 3,
        out_specs=(VMEM, VMEM),
        name="middle",
    )(residual, parts, gain.reshape(1, d))


def exchanged(blocks):
    return lax.all_to_all(blocks, "tp", 0, 0, tiled=True)


def attention(queries, key_heads, value_heads, documents, sink_logits):
    tok_rows = queries.shape[0]
    q_local = queries.shape[1] // HD
    kv_local = key_heads.shape[1] // HD
    groups = q_local // kv_local
    size = lax.axis_size("sp")
    own_docs = documents.astype(jnp.bfloat16)
    keys_values = jnp.concatenate([key_heads, value_heads], axis=1)
    width = keys_values.shape[1]

    def edge(lo):
        docs = jnp.broadcast_to(own_docs[lo : lo + WINDOW].reshape(-1, width), (16, width))
        return jnp.concatenate([keys_values[lo : lo + WINDOW], docs], axis=0)

    up = [(i, i + 1) for i in range(size - 1)]
    down = [(j, i) for i, j in up]
    before = lax.ppermute(edge(tok_rows - WINDOW), "sp", up)
    after = lax.ppermute(edge(0), "sp", down)
    spread = jnp.concatenate([before[:WINDOW], keys_values, after[:WINDOW]], axis=0)
    spread_docs = jnp.concatenate([before[WINDOW], own_docs, after[WINDOW]])
    spread_keys, spread_values = spread[:, : kv_local * HD], spread[:, kv_local * HD :]
    offset = lax.axis_index("sp") * tok_rows
    total_length = tok_rows * size
    query_pos = offset + jnp.arange(tok_rows, dtype=jnp.int32)
    key_pos = offset - WINDOW + jnp.arange(tok_rows + 2 * WINDOW, dtype=jnp.int32)
    allowed = (
        (jnp.abs(query_pos[:, None] - key_pos[None, :]) <= WINDOW)
        & (key_pos >= 0)[None, :]
        & (key_pos < total_length)[None, :]
        & (own_docs[:, None] == spread_docs[None, :])
    )
    query_block = queries.reshape(tok_rows, kv_local, groups, HD)
    key_block = spread_keys.reshape(-1, kv_local, HD)
    value_block = spread_values.reshape(-1, kv_local, HD)
    scores = jnp.einsum(
        "qkgd,jkd->kgqj", query_block, key_block, preferred_element_type=jnp.float32
    ) * HD ** (-0.5)
    scores = jnp.where(allowed[None, None], scores, masked)
    sink_table = sink_logits.reshape(kv_local, groups)[:, :, None]
    row_max = jnp.maximum(jnp.max(scores, axis=-1), sink_table)
    expo = jnp.exp(scores - row_max[..., None])
    total = jnp.sum(expo, axis=-1) + jnp.exp(sink_table - row_max)
    probs = (expo / total[..., None]).astype(jnp.bfloat16)
    mixed = jnp.einsum("kgqj,jkd->qkgd", probs, value_block, preferred_element_type=jnp.float32)
    return mixed.reshape(tok_rows, q_local * HD).astype(jnp.bfloat16)


def on_device(
    residual,
    queries,
    key_heads,
    value_heads,
    documents,
    sink_logits,
    out_weight,
    norm_gain,
    gate_weight,
    up_weight,
    down_weight,
):
    n_tp = lax.axis_size("tp")
    d = residual.shape[1]
    ring = Ring(pack(gate_weight, up_weight, down_weight))
    queries, ring.block = lax.optimization_barrier((queries, ring.block))
    ring.run()
    attended = attention(queries, key_heads, value_heads, documents, sink_logits)
    partial = jnp.dot(attended, out_weight, preferred_element_type=jnp.float32)
    parts = exchanged(split_up(partial.astype(jnp.bfloat16), n_tp))
    middle, copies = middle_and_normed(residual, parts, norm_gain)
    rows = exchanged(copies).reshape(-1, d)
    mixed = exchanged(split_up(ffn(rows, ring.kept, ring.swapped), n_tp))
    return finish(middle, [mixed])


def solution(mesh):
    return jax.shard_map(
        on_device,
        mesh=mesh,
        in_specs=(
            P(("grp", "sp", "tp"), None),
            P(("grp", "sp"), "tp"),
            P(("grp", "sp"), "tp"),
            P(("grp", "sp"), "tp"),
            P(("grp", "sp")),
            P("tp"),
            P("tp", None),
            P(),
            P("sp", "tp"),
            P("sp", "tp"),
            P("sp", "tp"),
        ),
        out_specs=P(("grp", "sp", "tp"), None),
        check_vma=False,
    )
```

```python
import functools

import jax
import jax.numpy as jnp
from jax import lax
from jax.experimental import pallas as pl
from jax.experimental.pallas import tpu as pltpu
from jax.sharding import PartitionSpec as P

HD = 64
WINDOW = 128
LANES = 128
TALL = 256
ROW_STEPS = 4
TILES = ((0, 512), (512, 1536), (1536, 2816))

epsilon = 1e-06
masked = -1e30

VMEM = pl.BlockSpec(memory_space=pltpu.VMEM)
HBM = pl.BlockSpec(memory_space=pl.ANY)
LIMIT = pltpu.CompilerParams(vmem_limit_bytes=56 * 1024 * 1024)


def split_up(shard, length):
    return shard.reshape(length, shard.shape[0] // length, *shard.shape[1:])


def pack_body(gate, up, down, out):
    ff = gate.shape[1]
    for i in range(ff // LANES):
        at = slice(i * LANES, (i + 1) * LANES)
        out[:, 2 * i * LANES : (2 * i + 1) * LANES] = gate[:, at]
        out[:, (2 * i + 1) * LANES : (2 * i + 2) * LANES] = up[:, at]
    out[:, 2 * ff :] = down[...]


def pack(gate, up, down):
    rows, ff = gate.shape
    return pl.pallas_call(
        pack_body,
        out_shape=jax.ShapeDtypeStruct((rows, 3 * ff), gate.dtype),
        in_specs=[VMEM] * 3,
        out_specs=VMEM,
        name="pack",
    )(gate, up, down)


def ffn_body(rows, w, out, x, wide, narrow, hidden, xsem, sems, dsems):
    tokens, d = x.shape
    ff = hidden.shape[1]
    loads = [
        pltpu.make_async_copy(w.at[:, a:b], wide.at[:, a:b], sems.at[k])
        for k, (a, b) in enumerate(TILES)
    ]
    half = d // 2
    later = [
        pltpu.make_async_copy(
            w.at[n * half : (n + 1) * half, 2 * ff :],
            narrow.at[n * half : (n + 1) * half],
            dsems.at[n],
        )
        for n in range(2)
    ]
    load_x = pltpu.make_async_copy(rows, x, xsem)
    load_x.start()
    for c in loads + later:
        c.start()
    load_x.wait()
    for c, (a, b) in zip(loads, TILES):
        c.wait()

        @pl.loop(0, tokens // TALL)
        def _(m, a=a, b=b):
            at = pl.ds(m * TALL, TALL)
            both = jnp.dot(x[at], wide[:, a:b], preferred_element_type=jnp.float32)
            for k in range((b - a) // (2 * LANES)):
                gate = both[:, 2 * k * LANES : (2 * k + 1) * LANES]
                up = both[:, (2 * k + 1) * LANES : (2 * k + 2) * LANES]
                lane = a // 2 + k * LANES
                hidden[at, lane : lane + LANES] = (gate / (1.0 + jnp.exp(-gate)) * up).astype(
                    hidden.dtype
                )

    for n, c in enumerate(later):
        c.wait()

        @pl.loop(0, tokens // TALL)
        def _(m, n=n):
            at = pl.ds(m * TALL, TALL)
            out[at, n * half : (n + 1) * half] = lax.dot_general(
                hidden[at],
                narrow[n * half : (n + 1) * half],
                (((1,), (1,)), ((), ())),
                preferred_element_type=jnp.float32,
            ).astype(out.dtype)


def ffn(rows, w):
    tokens, d = rows.shape
    ff = w.shape[1] // 3
    assert TILES[-1][1] == 2 * ff
    return pl.pallas_call(
        ffn_body,
        out_shape=jax.ShapeDtypeStruct((tokens, d), rows.dtype),
        in_specs=[HBM] * 2,
        out_specs=VMEM,
        scratch_shapes=[
            pltpu.VMEM((tokens, d), rows.dtype),
            pltpu.VMEM((d, 2 * ff), rows.dtype),
            pltpu.VMEM((d, ff), rows.dtype),
            pltpu.VMEM((tokens, ff), rows.dtype),
            pltpu.SemaphoreType.DMA,
            pltpu.SemaphoreType.DMA((len(TILES),)),
            pltpu.SemaphoreType.DMA((2,)),
        ],
        compiler_params=LIMIT,
        cost_estimate=pl.CostEstimate(
            flops=6 * tokens * ff * d, bytes_accessed=6 * d * ff + 4 * tokens * d, transcendentals=tokens * ff
        ),
        name="ffn",
    )(rows, w)


def finish_body(middle, parts, out):
    total = parts[0].astype(jnp.float32)
    for k in range(1, parts.shape[0]):
        total = total + parts[k].astype(jnp.float32)
    mixed = total.astype(jnp.bfloat16).astype(jnp.float32)
    out[...] = (middle[...].astype(jnp.float32) + 0.5 * mixed).astype(out.dtype)


def finish(middle, parts):
    rows, d = middle.shape
    tall = rows // ROW_STEPS
    one = pl.BlockSpec((tall, d), lambda i: (i, 0))
    all_parts = pl.BlockSpec((parts.shape[0], tall, d), lambda i: (0, i, 0))
    return pl.pallas_call(
        finish_body,
        grid=(ROW_STEPS,),
        out_shape=jax.ShapeDtypeStruct((rows, d), middle.dtype),
        in_specs=[one, all_parts],
        out_specs=one,
        name="finish",
    )(middle, parts)


def middle_body(residual, parts, gain, middle, normed):
    total = parts[0].astype(jnp.float32)
    for k in range(1, parts.shape[0]):
        total = total + parts[k].astype(jnp.float32)
    projected = total.astype(jnp.bfloat16).astype(jnp.float32)
    mid = (residual[...].astype(jnp.float32) + projected).astype(jnp.bfloat16)
    middle[...] = mid
    wide = mid.astype(jnp.float32)
    scaled = wide * lax.rsqrt(jnp.mean(wide * wide, axis=-1, keepdims=True) + epsilon)
    out = (scaled * gain[...].astype(jnp.float32)).astype(normed.dtype)
    for k in range(normed.shape[0]):
        normed[k] = out


def middle_and_normed(residual, parts, gain):
    rows, d = residual.shape
    tall = rows // ROW_STEPS
    one = pl.BlockSpec((tall, d), lambda i: (i, 0))
    all_parts = pl.BlockSpec((parts.shape[0], tall, d), lambda i: (0, i, 0))
    return pl.pallas_call(
        middle_body,
        grid=(ROW_STEPS,),
        out_shape=(
            jax.ShapeDtypeStruct((rows, d), residual.dtype),
            jax.ShapeDtypeStruct((parts.shape[0], rows, d), residual.dtype),
        ),
        in_specs=[one, all_parts, pl.BlockSpec((1, d), lambda i: (0, 0))],
        out_specs=(one, all_parts),
        name="middle",
    )(residual, parts, gain.reshape(1, d))


def exchanged(blocks):
    return lax.all_to_all(blocks, "tp", 0, 0, tiled=True)


def attention(queries, key_heads, value_heads, documents, sink_logits):
    tok_rows = queries.shape[0]
    q_local = queries.shape[1] // HD
    kv_local = key_heads.shape[1] // HD
    groups = q_local // kv_local
    size = lax.axis_size("sp")
    own_docs = documents.astype(jnp.bfloat16)
    keys_values = jnp.concatenate([key_heads, value_heads], axis=1)
    width = keys_values.shape[1]

    def edge(lo):
        docs = jnp.broadcast_to(own_docs[lo : lo + WINDOW].reshape(-1, width), (16, width))
        return jnp.concatenate([keys_values[lo : lo + WINDOW], docs], axis=0)

    up = [(i, i + 1) for i in range(size - 1)]
    down = [(j, i) for i, j in up]
    before = lax.ppermute(edge(tok_rows - WINDOW), "sp", up)
    after = lax.ppermute(edge(0), "sp", down)
    spread = jnp.concatenate([before[:WINDOW], keys_values, after[:WINDOW]], axis=0)
    spread_docs = jnp.concatenate([before[WINDOW], own_docs, after[WINDOW]])
    spread_keys, spread_values = spread[:, : kv_local * HD], spread[:, kv_local * HD :]
    offset = lax.axis_index("sp") * tok_rows
    total_length = tok_rows * size
    query_pos = offset + jnp.arange(tok_rows, dtype=jnp.int32)
    key_pos = offset - WINDOW + jnp.arange(tok_rows + 2 * WINDOW, dtype=jnp.int32)
    allowed = (
        (jnp.abs(query_pos[:, None] - key_pos[None, :]) <= WINDOW)
        & (key_pos >= 0)[None, :]
        & (key_pos < total_length)[None, :]
        & (own_docs[:, None] == spread_docs[None, :])
    )
    query_block = queries.reshape(tok_rows, kv_local, groups, HD)
    key_block = spread_keys.reshape(-1, kv_local, HD)
    value_block = spread_values.reshape(-1, kv_local, HD)
    scores = jnp.einsum(
        "qkgd,jkd->kgqj", query_block, key_block, preferred_element_type=jnp.float32
    ) * HD ** (-0.5)
    scores = jnp.where(allowed[None, None], scores, masked)
    sink_table = sink_logits.reshape(kv_local, groups)[:, :, None]
    row_max = jnp.maximum(jnp.max(scores, axis=-1), sink_table)
    expo = jnp.exp(scores - row_max[..., None])
    total = jnp.sum(expo, axis=-1) + jnp.exp(sink_table - row_max)
    probs = (expo / total[..., None]).astype(jnp.bfloat16)
    mixed = jnp.einsum("kgqj,jkd->qkgd", probs, value_block, preferred_element_type=jnp.float32)
    return mixed.reshape(tok_rows, q_local * HD).astype(jnp.bfloat16)


def on_device(
    residual,
    queries,
    key_heads,
    value_heads,
    documents,
    sink_logits,
    out_weight,
    norm_gain,
    gate_weight,
    up_weight,
    down_weight,
):
    n_tp = lax.axis_size("tp")
    d = residual.shape[1]
    whole = lax.all_gather(pack(gate_weight, up_weight, down_weight), "sp", axis=0, tiled=True)
    attended = attention(queries, key_heads, value_heads, documents, sink_logits)
    partial = jnp.dot(attended, out_weight, preferred_element_type=jnp.float32)
    parts = exchanged(split_up(partial.astype(jnp.bfloat16), n_tp))
    middle, copies = middle_and_normed(residual, parts, norm_gain)
    rows = exchanged(copies).reshape(-1, d)
    mixed = exchanged(split_up(ffn(rows, whole), n_tp))
    return finish(middle, mixed)


def solution(mesh):
    return jax.shard_map(
        on_device,
        mesh=mesh,
        in_specs=(
            P(("grp", "sp", "tp"), None),
            P(("grp", "sp"), "tp"),
            P(("grp", "sp"), "tp"),
            P(("grp", "sp"), "tp"),
            P(("grp", "sp")),
            P("tp"),
            P("tp", None),
            P(),
            P("sp", "tp"),
            P("sp", "tp"),
            P("sp", "tp"),
        ),
        out_specs=P(("grp", "sp", "tp"), None),
        check_vma=False,
    )
```

```python
import functools

import jax
import jax.numpy as jnp
from jax import lax
from jax.experimental import pallas as pl
from jax.experimental.pallas import tpu as pltpu
from jax.sharding import PartitionSpec as P

HD = 64
WINDOW = 128
LANES = 128
TALL = 256
TILES = ((0, 512), (512, 1536), (1536, 2816))

epsilon = 1e-06
masked = -1e30

VMEM = pl.BlockSpec(memory_space=pltpu.VMEM)
SMEM = pl.BlockSpec(memory_space=pltpu.SMEM)
HBM = pl.BlockSpec(memory_space=pl.ANY)
LIMIT = pltpu.CompilerParams(vmem_limit_bytes=56 * 1024 * 1024)


def split_up(shard, length):
    return shard.reshape(length, shard.shape[0] // length, *shard.shape[1:])


def pack_body(gate, up, down, out):
    ff = gate.shape[1]
    for i in range(ff // LANES):
        at = slice(i * LANES, (i + 1) * LANES)
        out[:, 2 * i * LANES : (2 * i + 1) * LANES] = gate[:, at]
        out[:, (2 * i + 1) * LANES : (2 * i + 2) * LANES] = up[:, at]
    out[:, 2 * ff :] = down[...]


def pack(gate, up, down):
    rows, ff = gate.shape
    return pl.pallas_call(
        pack_body,
        out_shape=jax.ShapeDtypeStruct((rows, 3 * ff), gate.dtype),
        in_specs=[VMEM] * 3,
        out_specs=VMEM,
        name="pack",
    )(gate, up, down)


def ffn_body(places, rows, w, out, x, wide, narrow, hidden, xsem, sems, dsems):
    tokens, d = x.shape
    ff = hidden.shape[1]
    tall = min(TALL, tokens)
    loads = [
        pltpu.make_async_copy(w.at[:, a:b], wide.at[:, a:b], sems.at[k])
        for k, (a, b) in enumerate(TILES)
    ]
    half = d // 2
    later = [
        pltpu.make_async_copy(
            w.at[n * half : (n + 1) * half, 2 * ff :],
            narrow.at[n * half : (n + 1) * half],
            dsems.at[n],
        )
        for n in range(2)
    ]
    each = rows.shape[1]
    x_loads = [
        pltpu.make_async_copy(rows.at[places[k]], x.at[k * each : (k + 1) * each], xsem.at[k])
        for k in range(tokens // each)
    ]
    for c in x_loads + loads + later:
        c.start()
    for c in x_loads:
        c.wait()
    for c, (a, b) in zip(loads, TILES):
        c.wait()

        @pl.loop(0, tokens // tall)
        def _(m, a=a, b=b):
            at = pl.ds(m * tall, tall)
            both = jnp.dot(x[at], wide[:, a:b], preferred_element_type=jnp.float32)
            for k in range((b - a) // (2 * LANES)):
                gate = both[:, 2 * k * LANES : (2 * k + 1) * LANES]
                up = both[:, (2 * k + 1) * LANES : (2 * k + 2) * LANES]
                lane = a // 2 + k * LANES
                hidden[at, lane : lane + LANES] = (gate / (1.0 + jnp.exp(-gate)) * up).astype(
                    hidden.dtype
                )

    for n, c in enumerate(later):
        c.wait()

        @pl.loop(0, tokens // tall)
        def _(m, n=n):
            at = pl.ds(m * tall, tall)
            out[at, n * half : (n + 1) * half] = lax.dot_general(
                hidden[at],
                narrow[n * half : (n + 1) * half],
                (((1,), (1,)), ((), ())),
                preferred_element_type=jnp.float32,
            ).astype(out.dtype)


def ffn(rows, w, blocks, name):
    _, each, d = rows.shape
    ff = w.shape[1] // 3
    tokens = each * len(blocks)
    assert TILES[-1][1] == 2 * ff
    return pl.pallas_call(
        ffn_body,
        out_shape=jax.ShapeDtypeStruct((tokens, d), rows.dtype),
        in_specs=[SMEM] + [HBM] * 2,
        out_specs=VMEM,
        scratch_shapes=[
            pltpu.VMEM((tokens, d), rows.dtype),
            pltpu.VMEM((d, 2 * ff), rows.dtype),
            pltpu.VMEM((d, ff), rows.dtype),
            pltpu.VMEM((tokens, ff), rows.dtype),
            pltpu.SemaphoreType.DMA((len(blocks),)),
            pltpu.SemaphoreType.DMA((len(TILES),)),
            pltpu.SemaphoreType.DMA((2,)),
        ],
        compiler_params=LIMIT,
        cost_estimate=pl.CostEstimate(
            flops=6 * tokens * ff * d, bytes_accessed=6 * d * ff + 4 * tokens * d, transcendentals=tokens * ff
        ),
        name=f"ffn_{name}",
    )(jnp.stack(blocks).astype(jnp.int32), rows, w)


def joined_body(near, half_up, half_down, up, down):
    rows, half = up.shape[0], half_up.shape[0]
    up[half:] = near[half:rows]
    up[:half] = (near[:half].astype(jnp.float32) + half_up[...].astype(jnp.float32)).astype(up.dtype)
    down[:half] = near[rows : rows + half]
    down[half:] = (near[rows + half :].astype(jnp.float32) + half_down[...].astype(jnp.float32)).astype(
        down.dtype
    )


def joined(near, half_up, half_down):
    out = jax.ShapeDtypeStruct((near.shape[0] // 2, near.shape[1]), near.dtype)
    return pl.pallas_call(
        joined_body,
        out_shape=(out, out),
        in_specs=[VMEM] * 3,
        out_specs=(VMEM, VMEM),
        name="joined",
    )(near, half_up, half_down)


def finish_body(middle, own, from_down, from_up, out):
    total = own[...].astype(jnp.float32) + from_down[...].astype(jnp.float32)
    total = total + from_up[...].astype(jnp.float32)
    mixed = total.astype(jnp.bfloat16).astype(jnp.float32)
    out[...] = (middle[...].astype(jnp.float32) + 0.5 * mixed).astype(out.dtype)


def finish(*arrays):
    return pl.pallas_call(
        finish_body,
        out_shape=jax.ShapeDtypeStruct(arrays[0].shape, arrays[0].dtype),
        in_specs=[VMEM] * len(arrays),
        out_specs=VMEM,
        name="finish",
    )(*arrays)


def mixed_into(middle, rows, w):
    size = lax.axis_size("tp")
    assert size == 4
    me = lax.axis_index("tp")
    up = [(i, (i + 1) % size) for i in range(size)]
    down = [(i, (i - 1) % size) for i in range(size)]
    half = rows.shape[1] // 2
    far = ffn(rows, w, [(me + 2) % size], "far")
    half_up = moved(far[:half], up, "half_up")
    half_down = moved(far[half:], down, "half_down")
    near = ffn(rows, w, [(me + 1) % size, (me + 3) % size], "near")
    to_up, to_down = joined(near, half_up, half_down)
    from_down = moved(to_up, up, "whole_up")
    from_up = moved(to_down, down, "whole_down")
    own = ffn(rows, w, [me], "own")
    return finish(middle, own, from_down, from_up)


def moved(block, perm, name):
    with jax.named_scope(name):
        return lax.ppermute(block, "tp", perm)


def middle_body(residual, parts, gain, middle, normed):
    total = parts[0].astype(jnp.float32)
    for k in range(1, parts.shape[0]):
        total = total + parts[k].astype(jnp.float32)
    projected = total.astype(jnp.bfloat16).astype(jnp.float32)
    mid = (residual[...].astype(jnp.float32) + projected).astype(jnp.bfloat16)
    middle[...] = mid
    wide = mid.astype(jnp.float32)
    scaled = wide * lax.rsqrt(jnp.mean(wide * wide, axis=-1, keepdims=True) + epsilon)
    out = (scaled * gain[...].astype(jnp.float32)).astype(normed.dtype)
    for k in range(normed.shape[0]):
        normed[k] = out


def middle_and_normed(residual, parts, gain):
    rows, d = residual.shape
    return pl.pallas_call(
        middle_body,
        out_shape=(
            jax.ShapeDtypeStruct((rows, d), residual.dtype),
            jax.ShapeDtypeStruct((parts.shape[0], rows, d), residual.dtype),
        ),
        in_specs=[VMEM] * 3,
        out_specs=(VMEM, VMEM),
        name="middle",
    )(residual, parts, gain.reshape(1, d))


def exchanged(blocks):
    return lax.all_to_all(blocks, "tp", 0, 0, tiled=True)


def attention(queries, key_heads, value_heads, documents, sink_logits):
    tok_rows = queries.shape[0]
    q_local = queries.shape[1] // HD
    kv_local = key_heads.shape[1] // HD
    groups = q_local // kv_local
    size = lax.axis_size("sp")
    own_docs = documents.astype(jnp.bfloat16)
    keys_values = jnp.concatenate([key_heads, value_heads], axis=1)
    width = keys_values.shape[1]

    def edge(lo):
        docs = jnp.broadcast_to(own_docs[lo : lo + WINDOW].reshape(-1, width), (16, width))
        return jnp.concatenate([keys_values[lo : lo + WINDOW], docs], axis=0)

    up = [(i, i + 1) for i in range(size - 1)]
    down = [(j, i) for i, j in up]
    before = lax.ppermute(edge(tok_rows - WINDOW), "sp", up)
    after = lax.ppermute(edge(0), "sp", down)
    spread = jnp.concatenate([before[:WINDOW], keys_values, after[:WINDOW]], axis=0)
    spread_docs = jnp.concatenate([before[WINDOW], own_docs, after[WINDOW]])
    spread_keys, spread_values = spread[:, : kv_local * HD], spread[:, kv_local * HD :]
    offset = lax.axis_index("sp") * tok_rows
    total_length = tok_rows * size
    query_pos = offset + jnp.arange(tok_rows, dtype=jnp.int32)
    key_pos = offset - WINDOW + jnp.arange(tok_rows + 2 * WINDOW, dtype=jnp.int32)
    allowed = (
        (jnp.abs(query_pos[:, None] - key_pos[None, :]) <= WINDOW)
        & (key_pos >= 0)[None, :]
        & (key_pos < total_length)[None, :]
        & (own_docs[:, None] == spread_docs[None, :])
    )
    query_block = queries.reshape(tok_rows, kv_local, groups, HD)
    key_block = spread_keys.reshape(-1, kv_local, HD)
    value_block = spread_values.reshape(-1, kv_local, HD)
    scores = jnp.einsum(
        "qkgd,jkd->kgqj", query_block, key_block, preferred_element_type=jnp.float32
    ) * HD ** (-0.5)
    scores = jnp.where(allowed[None, None], scores, masked)
    sink_table = sink_logits.reshape(kv_local, groups)[:, :, None]
    row_max = jnp.maximum(jnp.max(scores, axis=-1), sink_table)
    expo = jnp.exp(scores - row_max[..., None])
    total = jnp.sum(expo, axis=-1) + jnp.exp(sink_table - row_max)
    probs = (expo / total[..., None]).astype(jnp.bfloat16)
    mixed = jnp.einsum("kgqj,jkd->qkgd", probs, value_block, preferred_element_type=jnp.float32)
    return mixed.reshape(tok_rows, q_local * HD).astype(jnp.bfloat16)


def on_device(
    residual,
    queries,
    key_heads,
    value_heads,
    documents,
    sink_logits,
    out_weight,
    norm_gain,
    gate_weight,
    up_weight,
    down_weight,
):
    n_tp = lax.axis_size("tp")
    whole = lax.all_gather(pack(gate_weight, up_weight, down_weight), "sp", axis=0, tiled=True)
    attended = attention(queries, key_heads, value_heads, documents, sink_logits)
    partial = jnp.dot(attended, out_weight, preferred_element_type=jnp.float32)
    parts = exchanged(split_up(partial.astype(jnp.bfloat16), n_tp))
    middle, copies = middle_and_normed(residual, parts, norm_gain)
    return mixed_into(middle, exchanged(copies), whole)


def solution(mesh):
    return jax.shard_map(
        on_device,
        mesh=mesh,
        in_specs=(
            P(("grp", "sp", "tp"), None),
            P(("grp", "sp"), "tp"),
            P(("grp", "sp"), "tp"),
            P(("grp", "sp"), "tp"),
            P(("grp", "sp")),
            P("tp"),
            P("tp", None),
            P(),
            P("sp", "tp"),
            P("sp", "tp"),
            P("sp", "tp"),
        ),
        out_specs=P(("grp", "sp", "tp"), None),
        check_vma=False,
    )
```

```python
import functools

import jax
import jax.numpy as jnp
from jax import lax
from jax.experimental import pallas as pl
from jax.experimental.pallas import tpu as pltpu
from jax.sharding import PartitionSpec as P


HD = 64
WINDOW = 128
TALL = 256
TILES = ((0, 512), (512, 1408))

epsilon = 1e-06
masked = -1e30

VMEM = pl.BlockSpec(memory_space=pltpu.VMEM)
SMEM = pl.BlockSpec(memory_space=pltpu.SMEM)
HBM = pl.BlockSpec(memory_space=pl.ANY)
LIMIT = pltpu.CompilerParams(vmem_limit_bytes=56 * 1024 * 1024)


def split_up(shard, length):
    return shard.reshape(length, shard.shape[0] // length, *shard.shape[1:])


def pack_body(gate, up, down, out, sems):
    ff = gate.shape[1]
    copies = [
        pltpu.make_async_copy(weight, out.at[:, k * ff : (k + 1) * ff], sems.at[k])
        for k, weight in enumerate((gate, up, down))
    ]
    for c in copies:
        c.start()
    for c in copies:
        c.wait()


def pack(gate, up, down):
    rows, ff = gate.shape
    return pl.pallas_call(
        pack_body,
        out_shape=jax.ShapeDtypeStruct((rows, 3 * ff), gate.dtype),
        in_specs=[HBM] * 3,
        out_specs=VMEM,
        scratch_shapes=[pltpu.SemaphoreType.DMA((3,))],
        name="pack",
    )(gate, up, down)


def store_rows(outs, first, cols, value):
    each = outs[0].shape[0]
    for k in range(value.shape[0] // each):
        outs[first // each + k][:, cols] = value[k * each : (k + 1) * each].astype(outs[0].dtype)


def down_loads(w, narrow, sems):
    d, ff = narrow.shape
    half = d // 2
    return [
        pltpu.make_async_copy(
            w.at[n * half : (n + 1) * half, 2 * ff :],
            narrow.at[n * half : (n + 1) * half],
            sems.at[n],
        )
        for n in range(2)
    ]


def down_rows(loads, hidden, narrow, outs, rows):
    half = narrow.shape[0] // 2
    for n, c in enumerate(loads):
        c.wait()
        cols = slice(n * half, (n + 1) * half)
        part = lax.dot_general(
            hidden[0:rows], narrow[cols], (((1,), (1,)), ((), ())), preferred_element_type=jnp.float32
        )
        store_rows(outs, 0, cols, part)


def first_body(places, rows, w, hidden, low, high, x, gates, ups, narrow, xsem, sems, dsems):
    tokens = x.shape[0]
    each = rows.shape[1]
    ff = hidden.shape[1]
    loads = []
    for k, (a, b) in enumerate(TILES):
        loads += [
            pltpu.make_async_copy(w.at[:, a:b], gates.at[:, a:b], sems.at[0, k]),
            pltpu.make_async_copy(w.at[:, ff + a : ff + b], ups.at[:, a:b], sems.at[1, k]),
        ]
    later = down_loads(w, narrow, dsems)
    x_loads = [
        pltpu.make_async_copy(rows.at[places[k]], x.at[k * each : (k + 1) * each], xsem.at[k])
        for k in range(tokens // each)
    ]
    for c in x_loads + loads + later:
        c.start()
    for c in x_loads:
        c.wait()
    for k, (a, b) in enumerate(TILES):
        loads[2 * k].wait()
        loads[2 * k + 1].wait()
        for m in range(0, tokens, TALL):
            at = slice(m, m + TALL)
            gate = jnp.dot(x[at], gates[:, a:b], preferred_element_type=jnp.float32)
            up = jnp.dot(x[at], ups[:, a:b], preferred_element_type=jnp.float32)
            hidden[at, a:b] = (gate / (1.0 + jnp.exp(-gate)) * up).astype(hidden.dtype)
    down_rows(later, hidden, narrow, (low, high), each)


def ffn_first(rows, w, places):
    blocks, each, d = rows.shape
    ff = w.shape[1] // 3
    tokens = blocks * each
    assert TILES[-1][1] == ff
    part = jax.ShapeDtypeStruct((each // 2, d), rows.dtype)
    return pl.pallas_call(
        first_body,
        out_shape=(jax.ShapeDtypeStruct((tokens, ff), rows.dtype), part, part),
        in_specs=[SMEM] + [HBM] * 2,
        out_specs=(VMEM,) * 3,
        scratch_shapes=[
            pltpu.VMEM((tokens, d), rows.dtype),
            pltpu.VMEM((d, ff), rows.dtype),
            pltpu.VMEM((d, ff), rows.dtype),
            pltpu.VMEM((d, ff), rows.dtype),
            pltpu.SemaphoreType.DMA((blocks,)),
            pltpu.SemaphoreType.DMA((2, len(TILES))),
            pltpu.SemaphoreType.DMA((2,)),
        ],
        compiler_params=LIMIT,
        cost_estimate=pl.CostEstimate(
            flops=2 * ff * d * (2 * tokens + each), bytes_accessed=6 * d * ff + 4 * tokens * d, transcendentals=tokens * ff
        ),
        name="ffn_first",
    )(jnp.stack(places).astype(jnp.int32), rows, w)


def next_body(start, hidden, w, *refs):
    outs, (part, narrow, hsem, sems) = refs[:-4], refs[-4:]
    loads = down_loads(w, narrow, sems)
    load = pltpu.make_async_copy(hidden.at[start : start + part.shape[0]], part, hsem)
    load.start()
    for c in loads:
        c.start()
    load.wait()
    down_rows(loads, part, narrow, outs, part.shape[0])


def ffn_next(hidden, w, start, count, pieces):
    ff = hidden.shape[1]
    d = w.shape[0]
    out = jax.ShapeDtypeStruct((count // pieces, d), hidden.dtype)
    return pl.pallas_call(
        functools.partial(next_body, start),
        out_shape=(out,) * pieces,
        in_specs=[HBM] * 2,
        out_specs=(VMEM,) * pieces,
        scratch_shapes=[
            pltpu.VMEM((count, ff), hidden.dtype),
            pltpu.VMEM((d, ff), hidden.dtype),
            pltpu.SemaphoreType.DMA,
            pltpu.SemaphoreType.DMA((2,)),
        ],
        compiler_params=LIMIT,
        cost_estimate=pl.CostEstimate(
            flops=2 * count * ff * d, bytes_accessed=2 * (d + count) * ff + 2 * count * d, transcendentals=0
        ),
    )(hidden, w)


def wide_sum(*parts):
    total = parts[0].astype(jnp.float32)
    for part in parts[1:]:
        total = total + part.astype(jnp.float32)
    return total.astype(parts[0].dtype)


def mixed_into(middle, rows, w):
    size = lax.axis_size("tp")
    assert size == 4
    me = lax.axis_index("tp")
    up = [(i, (i + 1) % size) for i in range(size)]
    down = [(i, (i - 1) % size) for i in range(size)]
    each = rows.shape[1]
    places = [(me + k) % size for k in (2, 1, 3, 0)]
    hidden, far_low, far_high = ffn_first(rows, w, places)
    half_up = moved(far_low, up)
    half_down = moved(far_high, down)
    up_low, up_high, down_low, down_high = ffn_next(hidden, w, each, 2 * each, 4)
    plain_high = moved(up_high, up)
    plain_low = moved(down_low, down)
    joined_low = moved(wide_sum(up_low, half_up), up)
    joined_high = moved(wide_sum(down_high, half_down), down)
    own_low, own_high = ffn_next(hidden, w, 3 * each, each, 2)
    half = each // 2
    low = half_added(middle[:half], own_low, joined_low, plain_low)
    high = half_added(middle[half:], own_high, plain_high, joined_high)
    return jnp.concatenate([low, high], axis=0)


def half_added(middle, *parts):
    mixed = wide_sum(*parts).astype(jnp.float32)
    return (middle.astype(jnp.float32) + 0.5 * mixed).astype(middle.dtype)


def moved(block, perm):
    return lax.ppermute(block, "tp", perm)


def middle_body(residual, parts, gain, middle, normed):
    total = parts[0].astype(jnp.float32)
    for k in range(1, parts.shape[0]):
        total = total + parts[k].astype(jnp.float32)
    projected = total.astype(jnp.bfloat16).astype(jnp.float32)
    mid = (residual[...].astype(jnp.float32) + projected).astype(jnp.bfloat16)
    middle[...] = mid
    wide = mid.astype(jnp.float32)
    scaled = wide * lax.rsqrt(jnp.mean(wide * wide, axis=-1, keepdims=True) + epsilon)
    out = (scaled * gain[...].astype(jnp.float32)).astype(normed.dtype)
    for k in range(normed.shape[0]):
        normed[k] = out


def middle_and_normed(residual, parts, gain):
    rows, d = residual.shape
    return pl.pallas_call(
        middle_body,
        out_shape=(
            jax.ShapeDtypeStruct((rows, d), residual.dtype),
            jax.ShapeDtypeStruct((parts.shape[0], rows, d), residual.dtype),
        ),
        in_specs=[VMEM] * 3,
        out_specs=(VMEM, VMEM),
        name="middle",
    )(residual, parts, gain.reshape(1, d))


def exchanged(blocks):
    return lax.all_to_all(blocks, "tp", 0, 0, tiled=True)


def attention(queries, key_heads, value_heads, documents, sink_logits):
    tok_rows = queries.shape[0]
    q_local = queries.shape[1] // HD
    kv_local = key_heads.shape[1] // HD
    groups = q_local // kv_local
    size = lax.axis_size("sp")
    own_docs = documents.astype(jnp.bfloat16)
    keys_values = jnp.concatenate([key_heads, value_heads], axis=1)
    width = keys_values.shape[1]

    def edge(lo):
        docs = jnp.broadcast_to(own_docs[lo : lo + WINDOW].reshape(-1, width), (16, width))
        return jnp.concatenate([keys_values[lo : lo + WINDOW], docs], axis=0)

    up = [(i, i + 1) for i in range(size - 1)]
    down = [(j, i) for i, j in up]
    before = lax.ppermute(edge(tok_rows - WINDOW), "sp", up)
    after = lax.ppermute(edge(0), "sp", down)
    spread = jnp.concatenate([before[:WINDOW], keys_values, after[:WINDOW]], axis=0)
    spread_docs = jnp.concatenate([before[WINDOW], own_docs, after[WINDOW]])
    spread_keys, spread_values = spread[:, : kv_local * HD], spread[:, kv_local * HD :]
    offset = lax.axis_index("sp") * tok_rows
    total_length = tok_rows * size
    query_pos = offset + jnp.arange(tok_rows, dtype=jnp.int32)
    key_pos = offset - WINDOW + jnp.arange(tok_rows + 2 * WINDOW, dtype=jnp.int32)
    allowed = (
        (jnp.abs(query_pos[:, None] - key_pos[None, :]) <= WINDOW)
        & (key_pos >= 0)[None, :]
        & (key_pos < total_length)[None, :]
        & (own_docs[:, None] == spread_docs[None, :])
    )
    query_block = queries.reshape(tok_rows, kv_local, groups, HD)
    key_block = spread_keys.reshape(-1, kv_local, HD)
    value_block = spread_values.reshape(-1, kv_local, HD)
    scores = jnp.einsum(
        "qkgd,jkd->kgqj", query_block, key_block, preferred_element_type=jnp.float32
    ) * HD ** (-0.5)
    scores = jnp.where(allowed[None, None], scores, masked)
    sink_table = sink_logits.reshape(kv_local, groups)[:, :, None]
    row_max = jnp.maximum(jnp.max(scores, axis=-1), sink_table)
    expo = jnp.exp(scores - row_max[..., None])
    total = jnp.sum(expo, axis=-1) + jnp.exp(sink_table - row_max)
    probs = (expo / total[..., None]).astype(jnp.bfloat16)
    mixed = jnp.einsum("kgqj,jkd->qkgd", probs, value_block, preferred_element_type=jnp.float32)
    return mixed.reshape(tok_rows, q_local * HD).astype(jnp.bfloat16)


def on_device(
    residual,
    queries,
    key_heads,
    value_heads,
    documents,
    sink_logits,
    out_weight,
    norm_gain,
    gate_weight,
    up_weight,
    down_weight,
):
    n_tp = lax.axis_size("tp")
    whole = lax.all_gather(pack(gate_weight, up_weight, down_weight), "sp", axis=0, tiled=True)
    attended = attention(queries, key_heads, value_heads, documents, sink_logits)
    partial = jnp.dot(attended, out_weight, preferred_element_type=jnp.float32)
    parts = exchanged(split_up(partial.astype(jnp.bfloat16), n_tp))
    middle, copies = middle_and_normed(residual, parts, norm_gain)
    return mixed_into(middle, exchanged(copies), whole)


def solution(mesh):
    return jax.shard_map(
        on_device,
        mesh=mesh,
        in_specs=(
            P(("grp", "sp", "tp"), None),
            P(("grp", "sp"), "tp"),
            P(("grp", "sp"), "tp"),
            P(("grp", "sp"), "tp"),
            P(("grp", "sp")),
            P("tp"),
            P("tp", None),
            P(),
            P("sp", "tp"),
            P("sp", "tp"),
            P("sp", "tp"),
        ),
        out_specs=P(("grp", "sp", "tp"), None),
        check_vma=False,
    )
```

```python
import functools

import jax
import jax.numpy as jnp
from jax import lax
from jax.experimental import pallas as pl
from jax.experimental.pallas import tpu as pltpu
from jax.sharding import PartitionSpec as P


HD = 64
WINDOW = 128
LANES = 128
TALL = 256
TILES = ((0, 1024), (1024, 2816))

epsilon = 1e-06
masked = -1e30

VMEM = pl.BlockSpec(memory_space=pltpu.VMEM)
SMEM = pl.BlockSpec(memory_space=pltpu.SMEM)
HBM = pl.BlockSpec(memory_space=pl.ANY)
LIMIT = pltpu.CompilerParams(vmem_limit_bytes=56 * 1024 * 1024)


def split_up(shard, length):
    return shard.reshape(length, shard.shape[0] // length, *shard.shape[1:])


def pack_body(gate, up, down, out):
    ff = gate.shape[1]
    for i in range(ff // LANES):
        at = slice(i * LANES, (i + 1) * LANES)
        out[:, 2 * i * LANES : (2 * i + 1) * LANES] = gate[:, at]
        out[:, (2 * i + 1) * LANES : (2 * i + 2) * LANES] = up[:, at]
    out[:, 2 * ff :] = down[...]


def pack(gate, up, down):
    rows, ff = gate.shape
    return pl.pallas_call(
        pack_body,
        out_shape=jax.ShapeDtypeStruct((rows, 3 * ff), gate.dtype),
        in_specs=[VMEM] * 3,
        out_specs=VMEM,
        name="pack",
    )(gate, up, down)


def store_rows(outs, first, cols, value):
    each = outs[0].shape[0]
    for k in range(value.shape[0] // each):
        outs[first // each + k][:, cols] = value[k * each : (k + 1) * each].astype(outs[0].dtype)


def down_loads(w, narrow, sems):
    d, ff = narrow.shape
    half = d // 2
    return [
        pltpu.make_async_copy(
            w.at[n * half : (n + 1) * half, 2 * ff :],
            narrow.at[n * half : (n + 1) * half],
            sems.at[n],
        )
        for n in range(2)
    ]


def down_rows(loads, hidden, narrow, outs, rows):
    half = narrow.shape[0] // 2
    for n, c in enumerate(loads):
        c.wait()
        cols = slice(n * half, (n + 1) * half)
        part = lax.dot_general(
            hidden[0:rows], narrow[cols], (((1,), (1,)), ((), ())), preferred_element_type=jnp.float32
        )
        store_rows(outs, 0, cols, part)


def first_body(places, rows, w, hidden, low, high, x, wide, narrow, xsem, sems, dsems):
    tokens, _ = x.shape
    each = rows.shape[1]
    loads = [
        pltpu.make_async_copy(w.at[:, a:b], wide.at[:, a:b], sems.at[k])
        for k, (a, b) in enumerate(TILES)
    ]
    later = down_loads(w, narrow, dsems)
    x_loads = [
        pltpu.make_async_copy(rows.at[places[k]], x.at[k * each : (k + 1) * each], xsem.at[k])
        for k in range(tokens // each)
    ]
    for c in x_loads + loads + later:
        c.start()
    for c in x_loads:
        c.wait()
    for c, (a, b) in zip(loads, TILES):
        c.wait()

        @pl.loop(0, tokens // TALL)
        def _(m, a=a, b=b):
            at = pl.ds(m * TALL, TALL)
            both = jnp.dot(x[at], wide[:, a:b], preferred_element_type=jnp.float32)
            for k in range((b - a) // (2 * LANES)):
                gate = both[:, 2 * k * LANES : (2 * k + 1) * LANES]
                up = both[:, (2 * k + 1) * LANES : (2 * k + 2) * LANES]
                lane = a // 2 + k * LANES
                hidden[at, lane : lane + LANES] = (gate / (1.0 + jnp.exp(-gate)) * up).astype(
                    hidden.dtype
                )

    down_rows(later, hidden, narrow, (low, high), each)


def ffn_first(rows, w, places):
    blocks, each, d = rows.shape
    ff = w.shape[1] // 3
    tokens = blocks * each
    assert TILES[-1][1] == 2 * ff
    part = jax.ShapeDtypeStruct((each // 2, d), rows.dtype)
    return pl.pallas_call(
        first_body,
        out_shape=(jax.ShapeDtypeStruct((tokens, ff), rows.dtype), part, part),
        in_specs=[SMEM] + [HBM] * 2,
        out_specs=(VMEM,) * 3,
        scratch_shapes=[
            pltpu.VMEM((tokens, d), rows.dtype),
            pltpu.VMEM((d, 2 * ff), rows.dtype),
            pltpu.VMEM((d, ff), rows.dtype),
            pltpu.SemaphoreType.DMA((blocks,)),
            pltpu.SemaphoreType.DMA((len(TILES),)),
            pltpu.SemaphoreType.DMA((2,)),
        ],
        compiler_params=LIMIT,
        cost_estimate=pl.CostEstimate(
            flops=2 * ff * d * (2 * tokens + each), bytes_accessed=6 * d * ff + 4 * tokens * d, transcendentals=tokens * ff
        ),
        name="ffn_first",
    )(jnp.stack(places).astype(jnp.int32), rows, w)


def next_body(start, hidden, w, *refs):
    outs, (part, narrow, hsem, sems) = refs[:-4], refs[-4:]
    loads = down_loads(w, narrow, sems)
    load = pltpu.make_async_copy(hidden.at[start : start + part.shape[0]], part, hsem)
    load.start()
    for c in loads:
        c.start()
    load.wait()
    down_rows(loads, part, narrow, outs, part.shape[0])


def ffn_next(hidden, w, start, count, pieces):
    ff = hidden.shape[1]
    d = w.shape[0]
    out = jax.ShapeDtypeStruct((count // pieces, d), hidden.dtype)
    return pl.pallas_call(
        functools.partial(next_body, start),
        out_shape=(out,) * pieces,
        in_specs=[HBM] * 2,
        out_specs=(VMEM,) * pieces,
        scratch_shapes=[
            pltpu.VMEM((count, ff), hidden.dtype),
            pltpu.VMEM((d, ff), hidden.dtype),
            pltpu.SemaphoreType.DMA,
            pltpu.SemaphoreType.DMA((2,)),
        ],
        compiler_params=LIMIT,
        cost_estimate=pl.CostEstimate(
            flops=2 * count * ff * d, bytes_accessed=2 * (d + count) * ff + 2 * count * d, transcendentals=0
        ),
    )(hidden, w)


def wide_sum(*parts):
    total = parts[0].astype(jnp.float32)
    for part in parts[1:]:
        total = total + part.astype(jnp.float32)
    return total.astype(parts[0].dtype)


def mixed_into(middle, rows, w):
    size = lax.axis_size("tp")
    assert size == 4
    me = lax.axis_index("tp")
    up = [(i, (i + 1) % size) for i in range(size)]
    down = [(i, (i - 1) % size) for i in range(size)]
    each = rows.shape[1]
    places = [(me + k) % size for k in (2, 1, 3, 0)]
    hidden, far_low, far_high = ffn_first(rows, w, places)
    half_up = moved(far_low, up)
    half_down = moved(far_high, down)
    up_low, up_high, down_low, down_high = ffn_next(hidden, w, each, 2 * each, 4)
    plain_high = moved(up_high, up)
    plain_low = moved(down_low, down)
    joined_low = moved(wide_sum(up_low, half_up), up)
    joined_high = moved(wide_sum(down_high, half_down), down)
    own_low, own_high = ffn_next(hidden, w, 3 * each, each, 2)
    mixed = jnp.concatenate(
        [wide_sum(own_low, joined_low, plain_low), wide_sum(own_high, plain_high, joined_high)], axis=0
    )
    return (middle.astype(jnp.float32) + 0.5 * mixed.astype(jnp.float32)).astype(middle.dtype)


def moved(block, perm):
    return lax.ppermute(block, "tp", perm)


def middle_body(residual, parts, gain, middle, normed):
    total = parts[0].astype(jnp.float32)
    for k in range(1, parts.shape[0]):
        total = total + parts[k].astype(jnp.float32)
    projected = total.astype(jnp.bfloat16).astype(jnp.float32)
    mid = (residual[...].astype(jnp.float32) + projected).astype(jnp.bfloat16)
    middle[...] = mid
    wide = mid.astype(jnp.float32)
    scaled = wide * lax.rsqrt(jnp.mean(wide * wide, axis=-1, keepdims=True) + epsilon)
    out = (scaled * gain[...].astype(jnp.float32)).astype(normed.dtype)
    for k in range(normed.shape[0]):
        normed[k] = out


def middle_and_normed(residual, parts, gain):
    rows, d = residual.shape
    return pl.pallas_call(
        middle_body,
        out_shape=(
            jax.ShapeDtypeStruct((rows, d), residual.dtype),
            jax.ShapeDtypeStruct((parts.shape[0], rows, d), residual.dtype),
        ),
        in_specs=[VMEM] * 3,
        out_specs=(VMEM, VMEM),
        name="middle",
    )(residual, parts, gain.reshape(1, d))


def exchanged(blocks):
    return lax.all_to_all(blocks, "tp", 0, 0, tiled=True)


def attention(queries, key_heads, value_heads, documents, sink_logits):
    tok_rows = queries.shape[0]
    q_local = queries.shape[1] // HD
    kv_local = key_heads.shape[1] // HD
    groups = q_local // kv_local
    size = lax.axis_size("sp")
    own_docs = documents.astype(jnp.bfloat16)
    keys_values = jnp.concatenate([key_heads, value_heads], axis=1)
    width = keys_values.shape[1]

    def edge(lo):
        docs = jnp.broadcast_to(own_docs[lo : lo + WINDOW].reshape(-1, width), (16, width))
        return jnp.concatenate([keys_values[lo : lo + WINDOW], docs], axis=0)

    up = [(i, i + 1) for i in range(size - 1)]
    down = [(j, i) for i, j in up]
    before = lax.ppermute(edge(tok_rows - WINDOW), "sp", up)
    after = lax.ppermute(edge(0), "sp", down)
    spread = jnp.concatenate([before[:WINDOW], keys_values, after[:WINDOW]], axis=0)
    spread_docs = jnp.concatenate([before[WINDOW], own_docs, after[WINDOW]])
    spread_keys, spread_values = spread[:, : kv_local * HD], spread[:, kv_local * HD :]
    offset = lax.axis_index("sp") * tok_rows
    total_length = tok_rows * size
    query_pos = offset + jnp.arange(tok_rows, dtype=jnp.int32)
    key_pos = offset - WINDOW + jnp.arange(tok_rows + 2 * WINDOW, dtype=jnp.int32)
    allowed = (
        (jnp.abs(query_pos[:, None] - key_pos[None, :]) <= WINDOW)
        & (key_pos >= 0)[None, :]
        & (key_pos < total_length)[None, :]
        & (own_docs[:, None] == spread_docs[None, :])
    )
    query_block = queries.reshape(tok_rows, kv_local, groups, HD)
    key_block = spread_keys.reshape(-1, kv_local, HD)
    value_block = spread_values.reshape(-1, kv_local, HD)
    scores = jnp.einsum(
        "qkgd,jkd->kgqj", query_block, key_block, preferred_element_type=jnp.float32
    ) * HD ** (-0.5)
    scores = jnp.where(allowed[None, None], scores, masked)
    sink_table = sink_logits.reshape(kv_local, groups)[:, :, None]
    row_max = jnp.maximum(jnp.max(scores, axis=-1), sink_table)
    expo = jnp.exp(scores - row_max[..., None])
    total = jnp.sum(expo, axis=-1) + jnp.exp(sink_table - row_max)
    probs = (expo / total[..., None]).astype(jnp.bfloat16)
    mixed = jnp.einsum("kgqj,jkd->qkgd", probs, value_block, preferred_element_type=jnp.float32)
    return mixed.reshape(tok_rows, q_local * HD).astype(jnp.bfloat16)


def on_device(
    residual,
    queries,
    key_heads,
    value_heads,
    documents,
    sink_logits,
    out_weight,
    norm_gain,
    gate_weight,
    up_weight,
    down_weight,
):
    n_tp = lax.axis_size("tp")
    whole = lax.all_gather(pack(gate_weight, up_weight, down_weight), "sp", axis=0, tiled=True)
    attended = attention(queries, key_heads, value_heads, documents, sink_logits)
    partial = jnp.dot(attended, out_weight, preferred_element_type=jnp.float32)
    parts = exchanged(split_up(partial.astype(jnp.bfloat16), n_tp))
    middle, copies = middle_and_normed(residual, parts, norm_gain)
    return mixed_into(middle, exchanged(copies), whole)


def solution(mesh):
    return jax.shard_map(
        on_device,
        mesh=mesh,
        in_specs=(
            P(("grp", "sp", "tp"), None),
            P(("grp", "sp"), "tp"),
            P(("grp", "sp"), "tp"),
            P(("grp", "sp"), "tp"),
            P(("grp", "sp")),
            P("tp"),
            P("tp", None),
            P(),
            P("sp", "tp"),
            P("sp", "tp"),
            P("sp", "tp"),
        ),
        out_specs=P(("grp", "sp", "tp"), None),
        check_vma=False,
    )
```
